32 devices in a mesh: sp: 16 (over z, y, x), tp: 2 (over core).
Axes of the slice: x: 2, y: 2, z: 4, core: 2. Of those that a mesh axis runs over, the one named last changes fastest.
Arguments:
- residual: bfloat16 [4096, 2048], P(('sp', 'tp')), as said below
- outer_gate: bfloat16 [4096, 1024], P('sp', 'tp'), may hold values from -6 to 6
- conv_input: bfloat16 [4096, 1024], P('sp', 'tp'), as said below
- conv_value: bfloat16 [4096, 1024], P('sp', 'tp'), may hold values from -6 to 6
- doc_ids: int32 [4096], P('sp'), may hold values from 0 to 7, never falling along the last dimension, each value on 1 to 1024 neighbouring positions
- conv_taps: bfloat16 [3, 1024], P(None, 'tp'), may hold values from -3.5 to 3.5
- branch_gain: bfloat16 [1024], P('tp'), may hold values from 0.099609375 to 1.8984375
- out_weight: bfloat16 [1024, 2048], replicated, may hold values from -0.1875 to 0.1875
- ffn_gain: bfloat16 [2048], replicated, may hold values from 0.099609375 to 1.8984375
- route_ids: int32 [4096, 4], P(('sp', 'tp')), may hold values from 0 to 31, all different within a row; in each aligned block of 128 rows (0 to 127, 128 to 255, ...) at most 32 rows name the same one
- route_weight: float32 [4096, 4], P(('sp', 'tp')), may hold values from 0.2 to 1
- shared_gate: bfloat16 [2048, 512], replicated, may hold values from -0.125 to 0.125
- shared_up: bfloat16 [2048, 512], replicated, may hold values from -0.125 to 0.125
- shared_down: bfloat16 [512, 2048], replicated, may hold values from -0.25 to 0.25
- expert_gate: bfloat16 [32, 2048, 512], P(('sp', 'tp')), may hold values from -0.125 to 0.125
- expert_up: bfloat16 [32, 2048, 512], P(('sp', 'tp')), may hold values from -0.125 to 0.125
- expert_down: bfloat16 [32, 512, 2048], P(('sp', 'tp')), may hold values from -0.25 to 0.25
Outputs:
- layer_out: bfloat16 [4096, 2048], P(('sp', 'tp'))
The draws below stay inside these ranges and needn't reach their ends.
Inputs may be any that keep to these rules, and one draw needn't show every extreme that they name: `route_ids`: each row names 4 different experts. Within each aligned block of 128 rows (the rows of one device) no expert is named by more than 32 rows, and in every draw some expert is named by exactly 32 rows of some block. `doc_ids`: document numbers start at 0 and never fall along the sequence; each document has 1 to 1024 positions. `residual`: Real-valued, of order one. `conv_input`: Real-valued, of order one.
All inputs are finite; a program needn't handle non-finite values.
Results may differ from the reference program's by a relative error of at most 0.012.
Values may be sent and summed in bfloat16 or wider, within the bound.
A program may use at most 128 MiB of HBM per device.

```python
import math
import jax
import jax.numpy as jnp
import numpy as np
from jax import lax

D = 2048
CH = 1024
EFF = 512
SFF = 512
TAPS = 3
TOP = 4
TOK_DEV = 256
TOKENS = 4096
ROWS_DEV = 128
EXPERTS = 32
CAP = 32
DOCS = 8
N_TP = 2


def draw_residual(key, part):
    keys = jax.random.split(key, 2)
    base = jax.random.normal(keys[0], (TOKENS, D), jnp.float32)
    column_scale = jnp.exp(jax.random.uniform(keys[1], (1, D), jnp.float32, math.log(0.4), math.log(2.5)))
    values = base * column_scale
    return values.astype(jnp.bfloat16)


def draw_conv_input(key, part):
    keys = jax.random.split(key, 2)
    rising = jnp.exp(jnp.linspace(math.log(0.5), math.log(2.0), CH))[None, :]
    jitter = jax.random.uniform(keys[1], (1, CH), jnp.float32, 0.7, 1.4)
    base = jax.random.normal(keys[0], (TOKENS, CH), jnp.float32)
    values = base * rising * jitter
    return values.astype(jnp.bfloat16)


def shard_levels(stream_key, extent, shards, low, high):
    factor_of, own = 1.0, jax.random.fold_in(stream_key, 6)
    for dim, shards_of in shards:
        draws = jnp.exp(jax.random.uniform(jax.random.fold_in(own, dim), (shards_of,), jnp.float32, low / len(shards), high / len(shards)))
        factor_of = factor_of * jnp.repeat(draws, extent[dim] // shards_of).reshape([-1 if axis == dim else 1 for axis in range(len(extent))])
    return factor_of


def profile(number_of, total, most, lean):
    weights = [(1 << 20) // math.isqrt(standing ** lean) + 1 for standing in range(2, number_of + 1)]
    surplus, holding = total - most - (number_of - 1), [1] * (number_of - 1)
    while surplus > 0:
        movable = [i for i in range(number_of - 1) if holding[i] < most]
        mass, left = sum([weights[i] for i in movable]), surplus
        for i in movable:
            addition = min(most - holding[i], max(1, left * weights[i] // mass), surplus)
            holding[i] = holding[i] + addition
            surplus = surplus - addition
    return np.array([most] + holding)


def ragged_sizes(stream_key, number_of, total, bound, slope):
    if number_of == 2:
        one = jax.random.randint(stream_key, (), max(1, total - bound), min(bound, total - 1) + 1)
        return jnp.stack([one, total - one])
    tallies = jnp.asarray(profile(number_of, total, bound, slope), jnp.int32)
    pairs = (number_of - 1) // 2
    source_of, receiver = tallies[1:1 + 2 * pairs:2], tallies[2:2 + 2 * pairs:2]
    margin = jnp.minimum(source_of - 1, bound - receiver)
    shifted = jax.random.randint(jax.random.fold_in(stream_key, 1), (pairs,), 0, 1 << 20) % (margin + 1)
    tallies = tallies.at[1:1 + 2 * pairs:2].set(source_of - shifted).at[2:2 + 2 * pairs:2].set(receiver + shifted)
    return tallies[jax.random.permutation(jax.random.fold_in(stream_key, 2), number_of)]


def routed_block(stream_key, own, number, rows, number_of, top, bound, skew):
    order = jax.random.permutation(stream_key, number_of)
    heavy_load, usual = load_shares(number_of, rows * top, bound, skew, True), load_shares(number_of, rows * top, bound, skew, False)
    places = jnp.arange(number_of)

    def named(tallies, offset_by):
        used = int((tallies > 0).sum())
        fixed = max(1, used // 4)
        shifted = fixed + (places - fixed + offset_by * (used - fixed)) % max(1, number_of - fixed)
        return jnp.zeros((number_of,), jnp.int32).at[order[jnp.where(places < fixed, places, shifted)]].set(jnp.asarray(tallies, jnp.int32))

    tallies = jnp.where(number % 4 == 0, named(heavy_load, number // 4), named(usual, number - number // 4 - 1))
    mixed = jax.random.permutation(jax.random.fold_in(own, 3), number_of)
    donor, taker = mixed[0:number_of // 2 * 2:2], mixed[1:number_of // 2 * 2:2]
    margin = jnp.minimum(tallies[donor] - 1, bound - tallies[taker]) // 2
    margin = jnp.where((donor == order[0]) | (taker == order[0]) | (tallies[taker] == 0), 0, jnp.maximum(margin, 0))
    shifted = jax.random.randint(jax.random.fold_in(own, 4), (number_of // 2,), 0, 1 << 20) % (margin + 1)
    tallies = tallies.at[donor].add(-shifted).at[taker].add(shifted)
    items = jnp.searchsorted(jnp.cumsum(tallies), jnp.arange(rows * top), side="right").astype(jnp.int32)
    grid = items.reshape(top, rows).T
    grid = grid[jax.random.permutation(jax.random.fold_in(own, 1), rows)]
    offset_by = jax.random.randint(jax.random.fold_in(own, 2), (rows, 1), 0, top)
    return jnp.take_along_axis(grid, (jnp.arange(top)[None, :] + offset_by) % top, axis=1)


def load_shares(number_of, total, reach, skew, full):
    portions = [(1 << 20) // math.isqrt(grade ** skew) + 1 for grade in range(1, number_of + 1)]
    largest = reach if full else min(reach, max(-(-total // number_of), total * portions[0] // sum(portions)))
    least = 1 if total - largest >= number_of - 1 else 0
    holding, spare = [largest] + [least] * (number_of - 1), total - largest - least * (number_of - 1)
    while spare > 0:
        candidates = [i for i in range(1, number_of) if holding[i] < largest] or [i for i in range(1, number_of) if holding[i] < reach]
        pool, budget = sum([portions[i] for i in candidates]), spare
        for i in candidates:
            addition = min(reach - holding[i], max(1, budget * portions[i] // pool), spare)
            holding[i] = holding[i] + addition
            spare = spare - addition
    return np.array(holding)


def bell_draw(key, shape, scale, bound, cuts=(), kind=jnp.bfloat16):
    values = scale * jax.random.normal(key, shape, jnp.float32)
    if cuts:
        values = values * shard_levels(key, shape, cuts, -0.22, 0.18)
    return jnp.clip(values, -bound, bound).astype(kind)


def setup_inputs(seed: int = 0) -> dict:
    streams_of = jax.random.split(jax.random.key(seed), 18)
    residual = draw_residual(jax.random.fold_in(streams_of[17], 71), 0)
    outer_gate = bell_draw(streams_of[1], (TOKENS, CH), 1.0, 6.0, ((0, 16), (1, 2)))
    conv_input = draw_conv_input(jax.random.fold_in(streams_of[17], 71), 0)
    conv_value = bell_draw(streams_of[3], (TOKENS, CH), 1.0, 6.0, ((0, 16), (1, 2)))
    doc_ids = jnp.searchsorted(jnp.cumsum(ragged_sizes(streams_of[4], DOCS, TOKENS, 4 * TOK_DEV, 1)), jnp.arange(TOKENS), side="right").astype(jnp.int32)
    conv_taps = bell_draw(streams_of[5], (TAPS, CH), TAPS ** -0.5, 3.5, ((1, 2),))
    branch_gain = jnp.clip(1.0 + 0.18 * jax.random.normal(streams_of[6], (CH,), jnp.float32), 0.099609375, 1.8984375).astype(jnp.bfloat16)
    out_weight = bell_draw(streams_of[7], (CH, D), CH ** -0.5, 0.1875)
    ffn_gain = jnp.clip(1.0 + 0.18 * jax.random.normal(streams_of[8], (D,), jnp.float32), 0.099609375, 1.8984375).astype(jnp.bfloat16)
    route_ids_keys = jax.random.split(jax.random.fold_in(streams_of[9], 1), TOKENS // ROWS_DEV)
    route_ids_turns = jax.random.permutation(jax.random.fold_in(streams_of[9], 3), TOKENS // ROWS_DEV)
    route_ids = jax.vmap(lambda own, number: routed_block(jax.random.fold_in(streams_of[9], 2), own, number, ROWS_DEV, EXPERTS, TOP, CAP, 2))(route_ids_keys, route_ids_turns).reshape((TOKENS, TOP))
    route_weight = jnp.clip(0.2 + 0.8 * jax.random.uniform(streams_of[10], (TOKENS, TOP), jnp.float32) ** shard_levels(streams_of[10], (TOKENS, TOP), ((0, 32),), -0.2, 0.2), 0.2, 1.0)
    shared_gate = bell_draw(streams_of[11], (D, SFF), D ** -0.5, 0.125)
    shared_up = bell_draw(streams_of[12], (D, SFF), D ** -0.5, 0.125)
    shared_down = bell_draw(streams_of[13], (SFF, D), SFF ** -0.5, 0.25)
    expert_gate = bell_draw(streams_of[14], (EXPERTS, D, EFF), D ** -0.5, 0.125, ((0, 32),))
    expert_up = bell_draw(streams_of[15], (EXPERTS, D, EFF), D ** -0.5, 0.125, ((0, 32),))
    expert_down = bell_draw(streams_of[16], (EXPERTS, EFF, D), EFF ** -0.5, 0.25, ((0, 32),))
    return dict(residual=residual, outer_gate=outer_gate, conv_input=conv_input, conv_value=conv_value, doc_ids=doc_ids, conv_taps=conv_taps, branch_gain=branch_gain, out_weight=out_weight, ffn_gain=ffn_gain, route_ids=route_ids, route_weight=route_weight, shared_gate=shared_gate, shared_up=shared_up, shared_down=shared_down, expert_gate=expert_gate, expert_up=expert_up, expert_down=expert_down)


norm_eps = 1e-06

def reference(residual, outer_gate, conv_input, conv_value, doc_ids, conv_taps, branch_gain, out_weight, ffn_gain, route_ids, route_weight, shared_gate, shared_up, shared_down, expert_gate, expert_up, expert_down):
    source = conv_input.astype(jnp.float32) * conv_value.astype(jnp.float32)
    mixed_conv = jnp.zeros(source.shape, jnp.float32)
    for tap in range(TAPS):
        tap_lag = TAPS - 1 - tap
        lagged = jnp.pad(source, ((tap_lag, 0), (0, 0)))[:TOKENS]
        lagged_doc = jnp.pad(doc_ids, (tap_lag, 0), constant_values=-1)[:TOKENS]
        same_doc = (lagged_doc == doc_ids).astype(jnp.float32)[:, None]
        mixed_conv = mixed_conv + conv_taps[tap].astype(jnp.float32)[None, :] * lagged * same_doc
    branch = outer_gate.astype(jnp.float32) * mixed_conv
    inv_rms = lax.rsqrt(lax.optimization_barrier(jnp.mean(branch * branch, axis=1, keepdims=True)) + norm_eps)
    normed = (branch * inv_rms * branch_gain.astype(jnp.float32)[None, :]).astype(jnp.bfloat16)
    update = jnp.dot(normed, out_weight, preferred_element_type=jnp.float32)
    middle = (residual.astype(jnp.float32) + update).astype(jnp.bfloat16)
    mid_float = middle.astype(jnp.float32)
    mid_rms = lax.rsqrt(lax.optimization_barrier(jnp.mean(mid_float * mid_float, axis=1, keepdims=True)) + norm_eps)
    ffn_in = (mid_float * mid_rms * ffn_gain.astype(jnp.float32)[None, :]).astype(jnp.bfloat16)
    shared_hidden = (jax.nn.silu(jnp.dot(ffn_in, shared_gate, preferred_element_type=jnp.float32)) * jnp.dot(ffn_in, shared_up, preferred_element_type=jnp.float32)).astype(jnp.bfloat16)
    shared_out = jnp.dot(shared_hidden, shared_down, preferred_element_type=jnp.float32)
    block_rows = TOK_DEV // N_TP
    block_count = TOKENS // block_rows
    flat_expert = route_ids.reshape(block_count, block_rows * TOP)
    onehot = (flat_expert[:, :, None] == jnp.arange(EXPERTS, dtype=jnp.int32)[None, None, :]).astype(jnp.int32)
    slot_rank = lax.optimization_barrier(jnp.sum(onehot * (jnp.cumsum(onehot, axis=1) - onehot), axis=2))
    block_index = jnp.arange(block_count, dtype=jnp.int32)[:, None]
    slot_index = (flat_expert * (block_count * CAP) + block_index * CAP + slot_rank).reshape(-1)
    token_index = (jnp.arange(TOKENS * TOP, dtype=jnp.int32) // TOP).astype(jnp.int32)
    slot_token = jnp.full((EXPERTS * block_count * CAP,), TOKENS, jnp.int32).at[slot_index].set(token_index)
    slot_weight = jnp.zeros((EXPERTS * block_count * CAP,), jnp.float32).at[slot_index].set(route_weight.reshape(-1))
    slot_token = slot_token.reshape(EXPERTS, block_count * CAP)
    slot_weight = slot_weight.reshape(EXPERTS, block_count * CAP)
    padded_in = jnp.concatenate([ffn_in, jnp.zeros((1, D), jnp.bfloat16)], axis=0)

    def one_expert(total_sum, inputs):
        tokens_here, weights_here, gate_w, up_w, down_w = inputs
        gathered = padded_in[tokens_here]
        hidden = (jax.nn.silu(jnp.dot(gathered, gate_w, preferred_element_type=jnp.float32)) * jnp.dot(gathered, up_w, preferred_element_type=jnp.float32)).astype(jnp.bfloat16)
        result = jnp.dot(hidden, down_w, preferred_element_type=jnp.float32).astype(jnp.bfloat16)
        total_sum = total_sum.at[tokens_here].add(result.astype(jnp.float32) * weights_here[:, None])
        return (total_sum, None)
    routed, _ = lax.scan(one_expert, jnp.zeros((TOKENS + 1, D), jnp.float32), (slot_token, slot_weight, expert_gate, expert_up, expert_down))
    return (mid_float + shared_out + routed[:TOKENS]).astype(jnp.bfloat16)
```

```python
import functools

import jax
import jax.numpy as jnp
from jax import lax
from jax.experimental import pallas as pl
from jax.experimental.pallas import tpu as pltpu
from jax.sharding import PartitionSpec as P

norm_eps = 1e-06
MESH = pl.DeviceIdType.MESH
F32, BF16 = jnp.float32, jnp.bfloat16


def column_length(seq_devices):
    length = 1
    while length**3 < seq_devices:
        length *= 2
    return length


def from_behind(value, axis, by):
    peers = lax.axis_size(axis)
    pairs = [(i, i + by) for i in range(peers) if 0 <= i + by < peers]
    return lax.ppermute(value, axis, pairs)


def dot(a, b, contract=((1,), (0,))):
    return lax.dot_general(a, b, (contract, ((), ())), preferred_element_type=F32)


def experts_kernel(
    nz,
    plane,
    cores,
    slots,
    tops,
    x_hbm,
    meta_hbm,
    mid_hbm,
    sg_hbm,
    su_hbm,
    sd_hbm,
    eg_hbm,
    eu_hbm,
    ed_hbm,
    out_ref,
    gath,
    gmeta,
    sbuf,
    rbuf,
    res,
    back,
    zout,
    zin,
    acc,
    mid,
    sg,
    su,
    sd,
    eg,
    eu,
    ed,
    load_sem,
    own_send,
    own_meta_send,
    fwd_send,
    fwd_meta_send,
    z_recv,
    z_meta_recv,
    d_send,
    d_recv,
    b_send,
    b_recv,
    r_send,
    r_recv,
):
    me_sp, me_tp = lax.axis_index("sp"), lax.axis_index("tp")
    peers = plane * cores
    me_z, me_p = me_sp // plane, me_sp % plane
    me_q = me_p * cores + me_tp
    width = x_hbm.shape[1]

    def plane_dev(q):
        return (me_z * plane + q // cores, q % cores)

    def column_dev(z):
        return (z * plane + me_p, me_tp)

    loads = [
        pltpu.make_async_copy(src, dst, load_sem.at[i])
        for i, (src, dst) in enumerate(
            [
                (x_hbm, gath.at[me_z]),
                (meta_hbm, gmeta.at[me_z]),
                (mid_hbm, mid),
                (sg_hbm, sg),
                (su_hbm, su),
                (sd_hbm, sd),
                (eg_hbm, eg),
                (eu_hbm, eu),
                (ed_hbm, ed),
            ]
        )
    ]
    for load in loads:
        load.start()

    barrier = pltpu.get_barrier_semaphore()

    def greet_column(r, carry):
        pl.semaphore_signal(
            barrier, inc=1, device_id=column_dev((me_z + r) % nz), device_id_type=MESH
        )
        return carry

    def greet_plane(j, carry):
        pl.semaphore_signal(
            barrier, inc=1, device_id=plane_dev((me_q + j) % peers), device_id_type=MESH
        )
        return carry

    lax.fori_loop(1, nz, greet_column, 0)
    lax.fori_loop(1, peers, greet_plane, 0)
    pl.semaphore_wait(barrier, nz - 1 + peers - 1)

    def block_of(r):
        fewer = jnp.minimum(me_z, nz - 1 - me_z)
        paired = r <= 2 * fewer
        apart = jnp.where(paired, (r + 1) // 2, r - fewer)
        lower = jnp.where(paired, r % 2, jnp.where(me_z > nz - 1 - me_z, 1, 0))
        return jnp.where(lower == 1, me_z - apart, me_z + apart), lower

    def hop(z, target, send, meta_send):
        return (
            pltpu.make_async_remote_copy(
                gmeta.at[z], gmeta.at[z], meta_send, z_meta_recv.at[z], column_dev(target), MESH
            ),
            pltpu.make_async_remote_copy(
                gath.at[z], gath.at[z], send, z_recv.at[z], column_dev(target), MESH
            ),
        )

    loads[0].wait()
    loads[1].wait()

    def own_hops(act):
        @pl.when(me_z > 0)
        def _():
            for copy in hop(me_z, me_z - 1, own_send.at[0], own_meta_send.at[0]):
                act(copy)

        @pl.when(me_z < nz - 1)
        def _():
            for copy in hop(me_z, me_z + 1, own_send.at[1], own_meta_send.at[1]):
                act(copy)

    def forward_hops(r, act):
        z, lower = block_of(r)

        @pl.when((lower == 1) & (me_z < nz - 1))
        def _():
            for copy in hop(z, me_z + 1, fwd_send.at[r], fwd_meta_send.at[r]):
                act(copy)

        @pl.when((lower == 0) & (me_z > 0))
        def _():
            for copy in hop(z, me_z - 1, fwd_send.at[r], fwd_meta_send.at[r]):
                act(copy)

    own_hops(lambda copy: copy.start())

    def slot_match(z, k):
        first = me_z * peers * slots
        places = lax.broadcasted_iota(jnp.int32, (peers * slots, gmeta.shape[2]), 0) + first
        return places.astype(F32) == gmeta[z, k : k + 1, :]

    def out_copy(r, j):
        q = (me_q + j) % peers
        return pltpu.make_async_remote_copy(
            sbuf.at[r, q], rbuf.at[r, me_q], d_send.at[r, j], d_recv.at[r, j], plane_dev(q), MESH
        )

    def back_copy(r, j):
        q = (me_q + j) % peers
        return pltpu.make_async_remote_copy(
            res.at[r, q], back.at[r, me_q], b_send.at[r, j], b_recv.at[r, j], plane_dev(q), MESH
        )

    def return_copy(r):
        z, _ = block_of(r)
        return pltpu.make_async_remote_copy(
            zout.at[r], zin.at[me_z], r_send.at[r], r_recv.at[me_z], column_dev(z), MESH
        )

    def over_peers(act):
        def step(j, carry):
            act(j)
            return carry

        lax.fori_loop(1, peers, step, 0)

    def dispatch(r):
        z, _ = block_of(r)

        @pl.when(r > 0)
        def _():
            for copy in hop(z, me_z, fwd_send.at[r], fwd_meta_send.at[r]):
                copy.wait_recv()
            forward_hops(r, lambda copy: copy.start())

        pick = jnp.zeros((peers * slots, gmeta.shape[2]), F32)
        for k in range(tops):
            pick = jnp.where(slot_match(z, k), 1.0, pick)
        rows = dot(pick.astype(BF16), gath[z]).astype(BF16)
        sbuf[r] = rows.reshape(peers, slots, width)
        rbuf[r, me_q] = sbuf[r, me_q]
        over_peers(lambda j: out_copy(r, j).start())

    def apply(r):
        over_peers(lambda j: out_copy(r, j).wait_recv())
        rows = rbuf[r].reshape(peers * slots, width)
        gate = dot(rows, eg[0])
        hidden = (gate / (1.0 + jnp.exp(-gate)) * dot(rows, eu[0])).astype(BF16)
        res[r] = dot(hidden, ed[0]).astype(BF16).reshape(peers, slots, width)
        back[r, me_q] = res[r, me_q]
        over_peers(lambda j: back_copy(r, j).start())

    def collect(r):
        over_peers(lambda j: back_copy(r, j).wait_recv())
        z, _ = block_of(r)
        weight = jnp.zeros((peers * slots, gmeta.shape[2]), F32)
        for k in range(tops):
            weight = jnp.where(slot_match(z, k), gmeta[z, tops + k : tops + k + 1, :], weight)
        rows = back[r].reshape(peers * slots, width)
        total = dot(weight.astype(BF16), rows, ((0,), (0,)))

        @pl.when(r == 0)
        def _():
            acc[...] += total

        @pl.when(r > 0)
        def _():
            zout[r] = total.astype(BF16)
            return_copy(r).start()

    def step(i, carry):
        @pl.when(i < nz)
        def _():
            dispatch(i)

        @pl.when(i == 0)
        def _():
            for load in loads[2:6]:
                load.wait()
            rows = gath[me_z]
            gate = dot(rows, sg[...])
            hidden = (gate / (1.0 + jnp.exp(-gate)) * dot(rows, su[...])).astype(BF16)
            acc[...] = mid[...].astype(F32) + dot(hidden, sd[...])
            for load in loads[6:]:
                load.wait()

        @pl.when((i >= 1) & (i <= nz))
        def _():
            apply(i - 1)

        @pl.when(i >= 2)
        def _():
            collect(i - 2)

        return carry

    lax.fori_loop(0, nz + 2, step, 0)

    def settle(r, carry):
        z, _ = block_of(r)
        pltpu.make_async_remote_copy(
            zout.at[r], zin.at[z], r_send.at[r], r_recv.at[z], column_dev(z), MESH
        ).wait_recv()
        acc[...] += zin[z].astype(F32)
        return carry

    lax.fori_loop(1, nz, settle, 0)
    out_ref[...] = acc[...].astype(BF16)

    own_hops(lambda copy: copy.wait_send())

    def drain_column(r, carry):
        forward_hops(r, lambda copy: copy.wait_send())
        return_copy(r).wait_send()
        return carry

    lax.fori_loop(1, nz, drain_column, 0)

    def drain_plane(r, carry):
        over_peers(lambda j: out_copy(r, j).wait_send())
        over_peers(lambda j: back_copy(r, j).wait_send())
        return carry

    lax.fori_loop(0, nz, drain_plane, 0)


def run_experts(ffn_in, meta, middle, shared, routed, slots):
    rows, width = ffn_in.shape
    seq_devices, cores = lax.axis_size("sp"), lax.axis_size("tp")
    nz = column_length(seq_devices)
    plane = seq_devices // nz
    peers = plane * cores
    dma = pltpu.SemaphoreType.DMA
    tile = (nz, peers, slots, width)
    hbm = pl.BlockSpec(memory_space=pl.ANY)
    weights = [pltpu.VMEM(w.shape, w.dtype) for w in (*shared, *routed)]
    return pl.pallas_call(
        functools.partial(experts_kernel, nz, plane, cores, slots, meta.shape[0] // 2),
        out_shape=jax.ShapeDtypeStruct((rows, width), BF16),
        in_specs=[hbm] * 9,
        out_specs=pl.BlockSpec(memory_space=pltpu.VMEM),
        scratch_shapes=[
            pltpu.VMEM((nz, rows, width), BF16),
            pltpu.VMEM((nz, *meta.shape), F32),
            pltpu.VMEM(tile, BF16),
            pltpu.VMEM(tile, BF16),
            pltpu.VMEM(tile, BF16),
            pltpu.VMEM(tile, BF16),
            pltpu.VMEM((nz, rows, width), BF16),
            pltpu.VMEM((nz, rows, width), BF16),
            pltpu.VMEM((rows, width), F32),
            pltpu.VMEM((rows, width), BF16),
            *weights,
            dma((9,)),
            dma((2,)),
            dma((2,)),
            dma((nz,)),
            dma((nz,)),
            dma((nz,)),
            dma((nz,)),
            dma((nz, peers)),
            dma((nz, peers)),
            dma((nz, peers)),
            dma((nz, peers)),
            dma((nz,)),
            dma((nz,)),
        ],
        compiler_params=pltpu.CompilerParams(
            collective_id=0, has_side_effects=True, vmem_limit_bytes=67043328
        ),
    )(ffn_in, meta, middle, *shared, *routed)


def shards(
    residual,
    outer_gate,
    conv_input,
    conv_value,
    doc_ids,
    conv_taps,
    branch_gain,
    out_weight,
    ffn_gain,
    route_ids,
    route_weight,
    shared_gate,
    shared_up,
    shared_down,
    expert_gate,
    expert_up,
    expert_down,
):
    seq_rows = conv_input.shape[0]
    half_width = conv_input.shape[1]
    tap_count = conv_taps.shape[0]
    lead_rows = tap_count - 1
    doc_float = doc_ids.astype(jnp.float32)
    prev_input, prev_value, prev_doc = from_behind(
        (
            conv_input[seq_rows - lead_rows :],
            conv_value[seq_rows - lead_rows :],
            doc_float[seq_rows - lead_rows :].astype(jnp.bfloat16),
        ),
        "sp",
        1,
    )
    source = jnp.concatenate(
        [
            prev_input.astype(jnp.float32) * prev_value.astype(jnp.float32),
            conv_input.astype(jnp.float32) * conv_value.astype(jnp.float32),
        ],
        axis=0,
    )
    doc_extended = jnp.concatenate([prev_doc.astype(jnp.float32), doc_float], axis=0)
    mixed_conv = jnp.zeros((seq_rows, half_width), jnp.float32)
    for tap in range(tap_count):
        same_doc = (doc_extended[tap : tap + seq_rows] == doc_float).astype(jnp.float32)[:, None]
        mixed_conv = (
            mixed_conv
            + conv_taps[tap].astype(jnp.float32)[None, :] * source[tap : tap + seq_rows] * same_doc
        )
    branch = outer_gate.astype(jnp.float32) * mixed_conv
    square_total = lax.psum(jnp.sum(branch * branch, axis=1, keepdims=True), "tp")
    inv_rms = lax.rsqrt(square_total / (half_width * lax.axis_size("tp")) + norm_eps)
    normed = (branch * inv_rms * branch_gain.astype(jnp.float32)[None, :]).astype(jnp.bfloat16)
    local_rows = residual.shape[0]
    token_rows = lax.all_to_all(normed, "tp", split_axis=0, concat_axis=1, tiled=True)
    update = jnp.dot(token_rows, out_weight, preferred_element_type=jnp.float32)
    middle = (residual.astype(jnp.float32) + update).astype(jnp.bfloat16)
    mid_float = middle.astype(jnp.float32)
    mid_rms = lax.rsqrt(jnp.mean(mid_float * mid_float, axis=1, keepdims=True) + norm_eps)
    ffn_in = (mid_float * mid_rms * ffn_gain.astype(jnp.float32)[None, :]).astype(jnp.bfloat16)

    top_count = route_ids.shape[1]
    core_devices = lax.axis_size("tp")
    expert_count = lax.axis_size("sp") * core_devices
    capacity = local_rows * core_devices * top_count // expert_count
    slots = -(-capacity // 16) * 16
    ids = route_ids.T
    experts = jnp.arange(expert_count, dtype=jnp.int32)
    named = jnp.sum((ids[:, None, :] == experts[None, :, None]).astype(F32), axis=0)
    token = jnp.arange(local_rows, dtype=jnp.int32)
    before = (token[:, None] < token[None, :]).astype(BF16)
    earlier = jnp.dot(named.astype(BF16), before, preferred_element_type=F32)
    rank = jnp.sum(
        jnp.where(ids[:, None, :] == experts[None, :, None], earlier[None, :, :], 0.0), axis=1
    )
    places = ids.astype(F32) * slots + rank
    meta = jnp.concatenate([places, route_weight.T], axis=0)
    return run_experts(
        ffn_in,
        meta,
        middle,
        (shared_gate, shared_up, shared_down),
        (expert_gate, expert_up, expert_down),
        slots,
    )


def solution(mesh):
    placed = (
        P(("sp", "tp"), None),
        P("sp", "tp"),
        P("sp", "tp"),
        P("sp", "tp"),
        P("sp"),
        P(None, "tp"),
        P("tp"),
        P(),
        P(),
        P(("sp", "tp"), None),
        P(("sp", "tp"), None),
        P(),
        P(),
        P(),
        P(("sp", "tp"), None, None),
        P(("sp", "tp"), None, None),
        P(("sp", "tp"), None, None),
    )
    return jax.shard_map(
        shards, mesh=mesh, in_specs=placed, out_specs=P(("sp", "tp"), None), check_vma=False
    )
```

```python
import functools

import jax
import jax.numpy as jnp
from jax import lax
from jax.experimental import pallas as pl
from jax.experimental.pallas import tpu as pltpu
from jax.sharding import PartitionSpec as P

norm_eps = 1e-06
MESH = pl.DeviceIdType.MESH
F32, BF16 = jnp.float32, jnp.bfloat16


def column_length(seq_devices):
    length = 1
    while length**3 < seq_devices:
        length *= 2
    return length


def dot(a, b, contract=((1,), (0,))):
    return lax.dot_general(a, b, (contract, ((), ())), preferred_element_type=F32)


def experts_kernel(
    nz,
    plane,
    cores,
    slots,
    tops,
    expert_count,
    in_hbm,
    val_hbm,
    doc_hbm,
    route_hbm,
    outer_hbm,
    ow_hbm,
    residual_hbm,
    sg_hbm,
    su_hbm,
    sd_hbm,
    eg_hbm,
    eu_hbm,
    ed_hbm,
    taps_ref,
    branch_gain_ref,
    ffn_gain_ref,
    out_ref,
    conv_in,
    conv_val,
    docs,
    route,
    outer,
    ow,
    residual,
    source,
    halo_in,
    halo_val,
    halo_doc,
    scaled,
    squares,
    other_scaled,
    other_squares,
    gath,
    gmeta,
    sbuf,
    rbuf,
    res,
    back,
    zout,
    zin,
    acc,
    sg,
    su,
    sd,
    eg,
    eu,
    ed,
    load_sem,
    halo_send,
    halo_recv,
    half_send,
    half_recv,
    own_send,
    own_meta_send,
    fwd_send,
    fwd_meta_send,
    z_recv,
    z_meta_recv,
    d_send,
    d_recv,
    b_send,
    b_recv,
    r_send,
    r_recv,
):
    me_sp, me_tp = lax.axis_index("sp"), lax.axis_index("tp")
    peers = plane * cores
    me_z, me_p = me_sp // plane, me_sp % plane
    me_q = me_p * cores + me_tp
    width = residual.shape[1]
    seq_devices = nz * plane

    def plane_dev(q):
        return (me_z * plane + q // cores, q % cores)

    def column_dev(z):
        return (z * plane + me_p, me_tp)

    loads = [
        pltpu.make_async_copy(src, dst, load_sem.at[i])
        for i, (src, dst) in enumerate(
            [
                (in_hbm, conv_in),
                (val_hbm, conv_val),
                (doc_hbm, docs),
                (route_hbm, route),
                (outer_hbm, outer),
                (ow_hbm, ow),
                (residual_hbm, residual),
                (sg_hbm, sg),
                (su_hbm, su),
                (sd_hbm, sd),
                (eg_hbm, eg),
                (eu_hbm, eu),
                (ed_hbm, ed),
            ]
        )
    ]
    for load in loads:
        load.start()

    barrier = pltpu.get_barrier_semaphore()

    def greet_column(r, carry):
        pl.semaphore_signal(
            barrier, inc=1, device_id=column_dev((me_z + r) % nz), device_id_type=MESH
        )
        return carry

    def greet_plane(j, carry):
        pl.semaphore_signal(
            barrier, inc=1, device_id=plane_dev((me_q + j) % peers), device_id_type=MESH
        )
        return carry

    lax.fori_loop(1, nz, greet_column, 0)
    lax.fori_loop(1, peers, greet_plane, 0)
    ahead = ((me_sp + 1) % seq_devices, me_tp)
    behind = ((me_sp + seq_devices - 1) % seq_devices, me_tp)
    pl.semaphore_signal(barrier, inc=1, device_id=ahead, device_id_type=MESH)
    pl.semaphore_signal(barrier, inc=1, device_id=behind, device_id_type=MESH)
    for load in loads[:4]:
        load.wait()
    pl.semaphore_wait(barrier, nz - 1 + peers - 1 + 2)

    seq_rows, half_width = conv_in.shape
    lead, packed = halo_doc.shape[0], halo_in.shape[0]
    halo_copies = [
        pltpu.make_async_remote_copy(
            src.at[pl.ds(seq_rows - dst.shape[0], dst.shape[0])],
            dst,
            halo_send.at[i],
            halo_recv.at[i],
            ahead,
            MESH,
        )
        for i, (src, dst) in enumerate(
            [(conv_in, halo_in), (conv_val, halo_val), (docs, halo_doc)]
        )
    ]
    for copy in halo_copies:
        copy.start()

    rows_here = residual.shape[0]
    named_by = route[...].T
    experts = lax.broadcasted_iota(jnp.int32, (expert_count, rows_here), 0).astype(F32)
    matches = [experts == named_by[k : k + 1, :] for k in range(tops)]
    named = jnp.zeros((expert_count, rows_here), F32)
    for match in matches:
        named = jnp.where(match, 1.0, named)
    square = (rows_here, rows_here)
    before = lax.broadcasted_iota(jnp.int32, square, 0) < lax.broadcasted_iota(jnp.int32, square, 1)
    earlier = dot(named.astype(BF16), jnp.where(before, 1.0, 0.0).astype(BF16))
    for k, match in enumerate(matches):
        rank = jnp.sum(jnp.where(match, earlier, 0.0), axis=0, keepdims=True)
        gmeta[me_z, k : k + 1, :] = named_by[k : k + 1, :] * slots + rank
        gmeta[me_z, tops + k : tops + k + 1, :] = named_by[tops + k : tops + k + 1, :]

    source[lead:, :] = conv_in[...].astype(F32) * conv_val[...].astype(F32)
    for load in loads[4:7]:
        load.wait()
    for copy in halo_copies:
        copy.wait_recv()
    inner = me_sp > 0
    product = halo_in[...].astype(F32) * halo_val[...].astype(F32)
    source[:lead, :] = jnp.where(inner, product[packed - lead :, :], 0.0)
    doc_here = docs[...]
    doc_all = jnp.concatenate([jnp.where(inner, halo_doc[...], -1.0), doc_here], axis=0)
    tap_count = taps_ref.shape[0]
    lanes = docs.shape[1]
    same = []
    for tap in range(tap_count):
        first = lead - (tap_count - 1 - tap)
        same.append(doc_all[first : first + seq_rows, :] == doc_here)
    total_square = jnp.zeros((seq_rows, 1), F32)
    for column in range(0, half_width, lanes):
        part = slice(column, column + lanes)
        mixed = jnp.zeros((seq_rows, lanes), F32)
        for tap in range(tap_count):
            first = lead - (tap_count - 1 - tap)
            lagged = source[first : first + seq_rows, part]
            weight = taps_ref[tap : tap + 1, part].astype(F32)
            mixed = mixed + jnp.where(same[tap], weight * lagged, 0.0)
        branch = outer[:, part].astype(F32) * mixed
        total_square = total_square + jnp.sum(branch * branch, axis=1, keepdims=True)
        scaled[:, part] = (branch * branch_gain_ref[:, part].astype(F32)).astype(BF16)
    squares[...] = jnp.broadcast_to(total_square, squares.shape)

    other_tp = 1 - me_tp
    theirs = pl.ds(pl.multiple_of(other_tp * rows_here, rows_here), rows_here)
    mine = pl.ds(pl.multiple_of(me_tp * rows_here, rows_here), rows_here)
    half_copies = [
        pltpu.make_async_remote_copy(
            src.at[theirs], dst, half_send.at[i], half_recv.at[i], (me_sp, other_tp), MESH
        )
        for i, (src, dst) in enumerate([(scaled, other_scaled), (squares, other_squares)])
    ]
    for copy in half_copies:
        copy.start()
    my_weight = pl.ds(pl.multiple_of(me_tp * half_width, half_width), half_width)
    their_weight = pl.ds(pl.multiple_of(other_tp * half_width, half_width), half_width)
    acc[...] = dot(scaled[mine, :], ow[my_weight, :])
    for copy in half_copies:
        copy.wait_recv()
    square_total = (squares[mine, :] + other_squares[...])[:, :1]
    inv_rms = lax.rsqrt(square_total / (half_width * cores) + norm_eps)
    update = (acc[...] + dot(other_scaled[...], ow[their_weight, :])) * inv_rms
    middle = (residual[...].astype(F32) + update).astype(BF16).astype(F32)
    mid_rms = lax.rsqrt(jnp.mean(middle * middle, axis=1, keepdims=True) + norm_eps)
    acc[...] = middle
    gath[me_z] = (middle * mid_rms * ffn_gain_ref[...].astype(F32)).astype(BF16)

    def block_of(r):
        fewer = jnp.minimum(me_z, nz - 1 - me_z)
        paired = r <= 2 * fewer
        apart = jnp.where(paired, (r + 1) // 2, r - fewer)
        lower = jnp.where(paired, r % 2, jnp.where(me_z > nz - 1 - me_z, 1, 0))
        return jnp.where(lower == 1, me_z - apart, me_z + apart), lower

    def hop(z, target, send, meta_send):
        return (
            pltpu.make_async_remote_copy(
                gmeta.at[z], gmeta.at[z], meta_send, z_meta_recv.at[z], column_dev(target), MESH
            ),
            pltpu.make_async_remote_copy(
                gath.at[z], gath.at[z], send, z_recv.at[z], column_dev(target), MESH
            ),
        )

    def own_hops(act):
        @pl.when(me_z > 0)
        def _():
            for copy in hop(me_z, me_z - 1, own_send.at[0], own_meta_send.at[0]):
                act(copy)

        @pl.when(me_z < nz - 1)
        def _():
            for copy in hop(me_z, me_z + 1, own_send.at[1], own_meta_send.at[1]):
                act(copy)

    def forward_hops(r, act):
        z, lower = block_of(r)

        @pl.when((lower == 1) & (me_z < nz - 1))
        def _():
            for copy in hop(z, me_z + 1, fwd_send.at[r], fwd_meta_send.at[r]):
                act(copy)

        @pl.when((lower == 0) & (me_z > 0))
        def _():
            for copy in hop(z, me_z - 1, fwd_send.at[r], fwd_meta_send.at[r]):
                act(copy)

    own_hops(lambda copy: copy.start())

    def slot_match(z, k):
        first = me_z * peers * slots
        places = lax.broadcasted_iota(jnp.int32, (peers * slots, gmeta.shape[2]), 0) + first
        return places.astype(F32) == gmeta[z, k : k + 1, :]

    def out_copy(r, j):
        q = (me_q + j) % peers
        return pltpu.make_async_remote_copy(
            sbuf.at[r, q], rbuf.at[r, me_q], d_send.at[r, j], d_recv.at[r, j], plane_dev(q), MESH
        )

    def back_copy(r, j):
        q = (me_q + j) % peers
        return pltpu.make_async_remote_copy(
            res.at[r, q], back.at[r, me_q], b_send.at[r, j], b_recv.at[r, j], plane_dev(q), MESH
        )

    def return_copy(r):
        z, _ = block_of(r)
        return pltpu.make_async_remote_copy(
            zout.at[r], zin.at[me_z], r_send.at[r], r_recv.at[me_z], column_dev(z), MESH
        )

    def over_peers(act):
        def step(j, carry):
            act(j)
            return carry

        lax.fori_loop(1, peers, step, 0)

    def dispatch(r):
        z, _ = block_of(r)

        @pl.when(r > 0)
        def _():
            for copy in hop(z, me_z, fwd_send.at[r], fwd_meta_send.at[r]):
                copy.wait_recv()
            forward_hops(r, lambda copy: copy.start())

        pick = jnp.zeros((peers * slots, gmeta.shape[2]), F32)
        for k in range(tops):
            pick = jnp.where(slot_match(z, k), 1.0, pick)
        rows = dot(pick.astype(BF16), gath[z]).astype(BF16)
        sbuf[r] = rows.reshape(peers, slots, width)
        rbuf[r, me_q] = sbuf[r, me_q]
        over_peers(lambda j: out_copy(r, j).start())

    def apply(r):
        over_peers(lambda j: out_copy(r, j).wait_recv())
        rows = rbuf[r].reshape(peers * slots, width)
        gate = dot(rows, eg[0])
        hidden = (gate / (1.0 + jnp.exp(-gate)) * dot(rows, eu[0])).astype(BF16)
        res[r] = dot(hidden, ed[0]).astype(BF16).reshape(peers, slots, width)
        back[r, me_q] = res[r, me_q]

        @pl.when(r > 0)
        def _():
            over_peers(lambda j: back_copy(r, j).start())

        @pl.when(r == nz - 1)
        def _():
            over_peers(lambda j: back_copy(0, j).start())

    def collect(r):
        over_peers(lambda j: back_copy(r, j).wait_recv())
        z, _ = block_of(r)
        weight = jnp.zeros((peers * slots, gmeta.shape[2]), F32)
        for k in range(tops):
            weight = jnp.where(slot_match(z, k), gmeta[z, tops + k : tops + k + 1, :], weight)
        rows = back[r].reshape(peers * slots, width)
        total = dot(weight.astype(BF16), rows, ((0,), (0,)))

        @pl.when(r == 0)
        def _():
            acc[...] += total

        @pl.when(r > 0)
        def _():
            zout[r] = total.astype(BF16)
            return_copy(r).start()

    def step(i, carry):
        @pl.when(i < nz)
        def _():
            dispatch(i)

        @pl.when(i == 0)
        def _():
            for load in loads[7:10]:
                load.wait()
            rows = gath[me_z]
            gate = dot(rows, sg[...])
            hidden = (gate / (1.0 + jnp.exp(-gate)) * dot(rows, su[...])).astype(BF16)
            acc[...] += dot(hidden, sd[...])
            for load in loads[10:]:
                load.wait()

        @pl.when((i >= 1) & (i <= nz))
        def _():
            apply(i - 1)

        @pl.when(i >= 3)
        def _():
            collect((i - 2) % nz)

        return carry

    lax.fori_loop(0, nz + 3, step, 0)

    def settle(r, carry):
        z, _ = block_of(r)
        pltpu.make_async_remote_copy(
            zout.at[r], zin.at[z], r_send.at[r], r_recv.at[z], column_dev(z), MESH
        ).wait_recv()
        acc[...] += zin[z].astype(F32)
        return carry

    lax.fori_loop(1, nz, settle, 0)
    out_ref[...] = acc[...].astype(BF16)

    for copy in halo_copies + half_copies:
        copy.wait_send()
    own_hops(lambda copy: copy.wait_send())

    def drain_column(r, carry):
        forward_hops(r, lambda copy: copy.wait_send())
        return_copy(r).wait_send()
        return carry

    lax.fori_loop(1, nz, drain_column, 0)

    def drain_plane(r, carry):
        over_peers(lambda j: out_copy(r, j).wait_send())
        over_peers(lambda j: back_copy(r, j).wait_send())
        return carry

    lax.fori_loop(0, nz, drain_plane, 0)


def shards(
    residual,
    outer_gate,
    conv_input,
    conv_value,
    doc_ids,
    conv_taps,
    branch_gain,
    out_weight,
    ffn_gain,
    route_ids,
    route_weight,
    shared_gate,
    shared_up,
    shared_down,
    expert_gate,
    expert_up,
    expert_down,
):
    rows, width = residual.shape
    seq_rows, half_width = conv_input.shape
    tops = route_ids.shape[1]
    seq_devices, cores = lax.axis_size("sp"), lax.axis_size("tp")
    nz = column_length(seq_devices)
    plane = seq_devices // nz
    peers = plane * cores
    expert_count = seq_devices * cores
    capacity = rows * cores * tops // expert_count
    slots = -(-capacity // 16) * 16
    lanes = 128
    docs = jnp.broadcast_to(doc_ids.astype(F32)[:, None], (seq_rows, lanes))
    route = jnp.concatenate([route_ids.astype(F32), route_weight], axis=1)
    route = jnp.pad(route, ((0, 0), (0, lanes - 2 * tops)))
    streamed = (
        conv_input,
        conv_value,
        docs,
        route,
        outer_gate,
        out_weight,
        residual,
        shared_gate,
        shared_up,
        shared_down,
        expert_gate,
        expert_up,
        expert_down,
    )
    held = [pltpu.VMEM(a.shape, a.dtype) for a in streamed]
    small = (conv_taps, branch_gain[None, :], ffn_gain[None, :])
    dma = pltpu.SemaphoreType.DMA
    tile = (nz, peers, slots, width)
    lead, packed = 8, 16
    return pl.pallas_call(
        functools.partial(experts_kernel, nz, plane, cores, slots, tops, expert_count),
        out_shape=jax.ShapeDtypeStruct((rows, width), BF16),
        in_specs=[pl.BlockSpec(memory_space=pl.ANY)] * len(streamed)
        + [pl.BlockSpec(memory_space=pltpu.VMEM)] * len(small),
        out_specs=pl.BlockSpec(memory_space=pltpu.VMEM),
        scratch_shapes=[
            *held[:7],
            pltpu.VMEM((lead + seq_rows, half_width), F32),
            pltpu.VMEM((packed, half_width), BF16),
            pltpu.VMEM((packed, half_width), BF16),
            pltpu.VMEM((lead, lanes), F32),
            pltpu.VMEM((seq_rows, half_width), BF16),
            pltpu.VMEM((seq_rows, lanes), F32),
            pltpu.VMEM((rows, half_width), BF16),
            pltpu.VMEM((rows, lanes), F32),
            pltpu.VMEM((nz, rows, width), BF16),
            pltpu.VMEM((nz, 2 * tops, rows), F32),
            pltpu.VMEM(tile, BF16),
            pltpu.VMEM(tile, BF16),
            pltpu.VMEM(tile, BF16),
            pltpu.VMEM(tile, BF16),
            pltpu.VMEM((nz, rows, width), BF16),
            pltpu.VMEM((nz, rows, width), BF16),
            pltpu.VMEM((rows, width), F32),
            *held[7:],
            dma((len(streamed),)),
            dma((3,)),
            dma((3,)),
            dma((2,)),
            dma((2,)),
            dma((2,)),
            dma((2,)),
            dma((nz,)),
            dma((nz,)),
            dma((nz,)),
            dma((nz,)),
            dma((nz, peers)),
            dma((nz, peers)),
            dma((nz, peers)),
            dma((nz, peers)),
            dma((nz,)),
            dma((nz,)),
        ],
        compiler_params=pltpu.CompilerParams(
            collective_id=0, has_side_effects=True, vmem_limit_bytes=67043328
        ),
    )(*streamed, *small)


def solution(mesh):
    placed = (
        P(("sp", "tp"), None),
        P("sp", "tp"),
        P("sp", "tp"),
        P("sp", "tp"),
        P("sp"),
        P(None, "tp"),
        P("tp"),
        P(),
        P(),
        P(("sp", "tp"), None),
        P(("sp", "tp"), None),
        P(),
        P(),
        P(),
        P(("sp", "tp"), None, None),
        P(("sp", "tp"), None, None),
        P(("sp", "tp"), None, None),
    )
    return jax.shard_map(
        shards, mesh=mesh, in_specs=placed, out_specs=P(("sp", "tp"), None), check_vma=False
    )
```

```python
import functools

import jax
import jax.numpy as jnp
from jax import lax
from jax.experimental import pallas as pl
from jax.experimental.pallas import tpu as pltpu
from jax.sharding import PartitionSpec as P

norm_eps = 1e-06
MESH = pl.DeviceIdType.MESH
F32, BF16 = jnp.float32, jnp.bfloat16


def column_length(seq_devices):
    length = 1
    while length**3 < seq_devices:
        length *= 2
    return length


def dot(a, b, contract=((1,), (0,))):
    return lax.dot_general(a, b, (contract, ((), ())), preferred_element_type=F32)


def experts_kernel(
    nz,
    plane,
    cores,
    slots,
    tops,
    expert_count,
    in_hbm,
    val_hbm,
    doc_hbm,
    ids_hbm,
    weights_hbm,
    outer_hbm,
    ow_hbm,
    residual_hbm,
    sg_hbm,
    su_hbm,
    sd_hbm,
    eg_hbm,
    eu_hbm,
    ed_hbm,
    taps_ref,
    branch_gain_ref,
    ffn_gain_ref,
    out_ref,
    conv_in,
    conv_val,
    docs,
    ids,
    weights,
    outer,
    ow,
    residual,
    source,
    halo_in,
    halo_val,
    halo_doc,
    scaled,
    squares,
    other_scaled,
    other_squares,
    gath,
    gmeta,
    sbuf,
    rbuf,
    res,
    back,
    zout,
    zin,
    acc,
    sg,
    su,
    sd,
    eg,
    eu,
    ed,
    load_sem,
    halo_send,
    halo_recv,
    half_send,
    half_recv,
    own_send,
    own_meta_send,
    fwd_send,
    fwd_meta_send,
    z_recv,
    z_meta_recv,
    d_send,
    d_recv,
    b_send,
    b_recv,
    r_send,
    r_recv,
):
    me_sp, me_tp = lax.axis_index("sp"), lax.axis_index("tp")
    peers = plane * cores
    me_z, me_p = me_sp // plane, me_sp % plane
    me_q = me_p * cores + me_tp
    width = residual.shape[1]
    seq_devices = nz * plane

    def plane_dev(q):
        return (me_z * plane + q // cores, q % cores)

    def column_dev(z):
        return (z * plane + me_p, me_tp)

    loads = [
        pltpu.make_async_copy(src, dst, load_sem.at[i])
        for i, (src, dst) in enumerate(
            [
                (in_hbm, conv_in),
                (val_hbm, conv_val),
                (doc_hbm, docs),
                (ids_hbm, ids),
                (weights_hbm, weights),
                (outer_hbm, outer),
                (ow_hbm, ow),
                (residual_hbm, residual),
                (sg_hbm, sg),
                (su_hbm, su),
                (sd_hbm, sd),
                (eg_hbm, eg),
                (eu_hbm, eu),
                (ed_hbm, ed),
            ]
        )
    ]
    for load in loads:
        load.start()

    barrier = pltpu.get_barrier_semaphore()

    def greet_column(r, carry):
        pl.semaphore_signal(
            barrier, inc=1, device_id=column_dev((me_z + r) % nz), device_id_type=MESH
        )
        return carry

    def greet_plane(j, carry):
        pl.semaphore_signal(
            barrier, inc=1, device_id=plane_dev((me_q + j) % peers), device_id_type=MESH
        )
        return carry

    lax.fori_loop(1, nz, greet_column, 0)
    lax.fori_loop(1, peers, greet_plane, 0)
    ahead = ((me_sp + 1) % seq_devices, me_tp)
    behind = ((me_sp + seq_devices - 1) % seq_devices, me_tp)
    pl.semaphore_signal(barrier, inc=1, device_id=ahead, device_id_type=MESH)
    pl.semaphore_signal(barrier, inc=1, device_id=behind, device_id_type=MESH)
    for load in loads[:5]:
        load.wait()
    pl.semaphore_wait(barrier, nz - 1 + peers - 1 + 2)

    seq_rows, half_width = conv_in.shape
    lead, packed = halo_doc.shape[0], halo_in.shape[0]
    halo_copies = [
        pltpu.make_async_remote_copy(
            src.at[pl.ds(seq_rows - dst.shape[0], dst.shape[0])],
            dst,
            halo_send.at[i],
            halo_recv.at[i],
            ahead,
            MESH,
        )
        for i, (src, dst) in enumerate(
            [(conv_in, halo_in), (conv_val, halo_val), (docs, halo_doc)]
        )
    ]
    for copy in halo_copies:
        copy.start()

    rows_here = residual.shape[0]
    named_by = ids[...].astype(F32)
    experts = lax.broadcasted_iota(jnp.int32, (expert_count, rows_here), 0).astype(F32)
    matches = [experts == named_by[k : k + 1, :] for k in range(tops)]
    named = jnp.zeros((expert_count, rows_here), F32)
    for match in matches:
        named = jnp.where(match, 1.0, named)
    square = (rows_here, rows_here)
    before = lax.broadcasted_iota(jnp.int32, square, 0) < lax.broadcasted_iota(jnp.int32, square, 1)
    earlier = dot(named.astype(BF16), jnp.where(before, 1.0, 0.0).astype(BF16))
    for k, match in enumerate(matches):
        rank = jnp.sum(jnp.where(match, earlier, 0.0), axis=0, keepdims=True)
        gmeta[me_z, k : k + 1, :] = named_by[k : k + 1, :] * slots + rank
        gmeta[me_z, tops + k : tops + k + 1, :] = weights[k : k + 1, :]

    source[lead:, :] = conv_in[...].astype(F32) * conv_val[...].astype(F32)
    for load in loads[5:8]:
        load.wait()
    for copy in halo_copies:
        copy.wait_recv()
    inner = me_sp > 0
    product = halo_in[...].astype(F32) * halo_val[...].astype(F32)
    source[:lead, :] = jnp.where(inner, product[packed - lead :, :], 0.0)
    doc_here = docs[...]
    doc_all = jnp.concatenate([jnp.where(inner, halo_doc[...], -1.0), doc_here], axis=0)
    tap_count = taps_ref.shape[0]
    lanes = docs.shape[1]
    same = []
    for tap in range(tap_count):
        first = lead - (tap_count - 1 - tap)
        same.append(doc_all[first : first + seq_rows, :] == doc_here)
    total_square = jnp.zeros((seq_rows, 1), F32)
    for column in range(0, half_width, lanes):
        part = slice(column, column + lanes)
        mixed = jnp.zeros((seq_rows, lanes), F32)
        for tap in range(tap_count):
            first = lead - (tap_count - 1 - tap)
            lagged = source[first : first + seq_rows, part]
            weight = taps_ref[tap : tap + 1, part].astype(F32)
            mixed = mixed + jnp.where(same[tap], weight * lagged, 0.0)
        branch = outer[:, part].astype(F32) * mixed
        total_square = total_square + jnp.sum(branch * branch, axis=1, keepdims=True)
        scaled[:, part] = (branch * branch_gain_ref[part].astype(F32)[None, :]).astype(BF16)
    squares[...] = jnp.broadcast_to(total_square, squares.shape)

    other_tp = 1 - me_tp
    theirs = pl.ds(pl.multiple_of(other_tp * rows_here, rows_here), rows_here)
    mine = pl.ds(pl.multiple_of(me_tp * rows_here, rows_here), rows_here)
    half_copies = [
        pltpu.make_async_remote_copy(
            src.at[theirs], dst, half_send.at[i], half_recv.at[i], (me_sp, other_tp), MESH
        )
        for i, (src, dst) in enumerate([(scaled, other_scaled), (squares, other_squares)])
    ]
    for copy in half_copies:
        copy.start()
    my_weight = pl.ds(pl.multiple_of(me_tp * half_width, half_width), half_width)
    their_weight = pl.ds(pl.multiple_of(other_tp * half_width, half_width), half_width)
    acc[...] = dot(scaled[mine, :], ow[my_weight, :])
    for copy in half_copies:
        copy.wait_recv()
    square_total = (squares[mine, :] + other_squares[...])[:, :1]
    inv_rms = lax.rsqrt(square_total / (half_width * cores) + norm_eps)
    update = (acc[...] + dot(other_scaled[...], ow[their_weight, :])) * inv_rms
    middle = (residual[...].astype(F32) + update).astype(BF16).astype(F32)
    mid_rms = lax.rsqrt(jnp.mean(middle * middle, axis=1, keepdims=True) + norm_eps)
    acc[...] = middle
    gath[me_z] = (middle * mid_rms * ffn_gain_ref[...].astype(F32)[None, :]).astype(BF16)

    def block_of(r):
        fewer = jnp.minimum(me_z, nz - 1 - me_z)
        paired = r <= 2 * fewer
        apart = jnp.where(paired, (r + 1) // 2, r - fewer)
        lower = jnp.where(paired, r % 2, jnp.where(me_z > nz - 1 - me_z, 1, 0))
        return jnp.where(lower == 1, me_z - apart, me_z + apart), lower

    def hop(z, target, send, meta_send):
        return (
            pltpu.make_async_remote_copy(
                gmeta.at[z], gmeta.at[z], meta_send, z_meta_recv.at[z], column_dev(target), MESH
            ),
            pltpu.make_async_remote_copy(
                gath.at[z], gath.at[z], send, z_recv.at[z], column_dev(target), MESH
            ),
        )

    def own_hops(act):
        @pl.when(me_z > 0)
        def _():
            for copy in hop(me_z, me_z - 1, own_send.at[0], own_meta_send.at[0]):
                act(copy)

        @pl.when(me_z < nz - 1)
        def _():
            for copy in hop(me_z, me_z + 1, own_send.at[1], own_meta_send.at[1]):
                act(copy)

    def forward_hops(r, act):
        z, lower = block_of(r)

        @pl.when((lower == 1) & (me_z < nz - 1))
        def _():
            for copy in hop(z, me_z + 1, fwd_send.at[r], fwd_meta_send.at[r]):
                act(copy)

        @pl.when((lower == 0) & (me_z > 0))
        def _():
            for copy in hop(z, me_z - 1, fwd_send.at[r], fwd_meta_send.at[r]):
                act(copy)

    own_hops(lambda copy: copy.start())

    def slot_match(z, k):
        first = me_z * peers * slots
        places = lax.broadcasted_iota(jnp.int32, (peers * slots, gmeta.shape[2]), 0) + first
        return places.astype(F32) == gmeta[z, k : k + 1, :]

    def out_copy(r, j):
        q = (me_q + j) % peers
        return pltpu.make_async_remote_copy(
            sbuf.at[r, q], rbuf.at[r, me_q], d_send.at[r, j], d_recv.at[r, j], plane_dev(q), MESH
        )

    def back_copy(r, j):
        q = (me_q + j) % peers
        return pltpu.make_async_remote_copy(
            res.at[r, q], back.at[r, me_q], b_send.at[r, j], b_recv.at[r, j], plane_dev(q), MESH
        )

    def return_copy(r):
        z, _ = block_of(r)
        return pltpu.make_async_remote_copy(
            zout.at[r], zin.at[me_z], r_send.at[r], r_recv.at[me_z], column_dev(z), MESH
        )

    def over_peers(act):
        def step(j, carry):
            act(j)
            return carry

        lax.fori_loop(1, peers, step, 0)

    def dispatch(r):
        z, _ = block_of(r)

        @pl.when(r > 0)
        def _():
            for copy in hop(z, me_z, fwd_send.at[r], fwd_meta_send.at[r]):
                copy.wait_recv()
            forward_hops(r, lambda copy: copy.start())

        pick = jnp.zeros((peers * slots, gmeta.shape[2]), F32)
        for k in range(tops):
            pick = jnp.where(slot_match(z, k), 1.0, pick)
        rows = dot(pick.astype(BF16), gath[z]).astype(BF16)
        sbuf[r] = rows.reshape(peers, slots, width)
        rbuf[r, me_q] = sbuf[r, me_q]
        over_peers(lambda j: out_copy(r, j).start())

    def apply(r):
        over_peers(lambda j: out_copy(r, j).wait_recv())
        rows = rbuf[r].reshape(peers * slots, width)
        gate = dot(rows, eg[0])
        hidden = (gate / (1.0 + jnp.exp(-gate)) * dot(rows, eu[0])).astype(BF16)
        res[r] = dot(hidden, ed[0]).astype(BF16).reshape(peers, slots, width)
        back[r, me_q] = res[r, me_q]

        @pl.when(r > 0)
        def _():
            over_peers(lambda j: back_copy(r, j).start())

        @pl.when(r == nz - 1)
        def _():
            over_peers(lambda j: back_copy(0, j).start())

    def collect(r):
        over_peers(lambda j: back_copy(r, j).wait_recv())
        z, _ = block_of(r)
        weight = jnp.zeros((peers * slots, gmeta.shape[2]), F32)
        for k in range(tops):
            weight = jnp.where(slot_match(z, k), gmeta[z, tops + k : tops + k + 1, :], weight)
        rows = back[r].reshape(peers * slots, width)
        total = dot(weight.astype(BF16), rows, ((0,), (0,)))

        @pl.when(r == 0)
        def _():
            acc[...] += total

        @pl.when(r > 0)
        def _():
            zout[r] = total.astype(BF16)
            return_copy(r).start()

    def step(i, carry):
        @pl.when(i < nz)
        def _():
            dispatch(i)

        @pl.when(i == 0)
        def _():
            for load in loads[8:11]:
                load.wait()
            rows = gath[me_z]
            gate = dot(rows, sg[...])
            hidden = (gate / (1.0 + jnp.exp(-gate)) * dot(rows, su[...])).astype(BF16)
            acc[...] += dot(hidden, sd[...])
            for load in loads[11:]:
                load.wait()

        @pl.when((i >= 1) & (i <= nz))
        def _():
            apply(i - 1)

        @pl.when(i >= 3)
        def _():
            collect((i - 2) % nz)

        return carry

    lax.fori_loop(0, nz + 3, step, 0)

    def settle(r, carry):
        z, _ = block_of(r)
        pltpu.make_async_remote_copy(
            zout.at[r], zin.at[z], r_send.at[r], r_recv.at[z], column_dev(z), MESH
        ).wait_recv()
        acc[...] += zin[z].astype(F32)
        return carry

    lax.fori_loop(1, nz, settle, 0)
    out_ref[...] = acc[...].astype(BF16)

    for copy in halo_copies + half_copies:
        copy.wait_send()
    own_hops(lambda copy: copy.wait_send())

    def drain_column(r, carry):
        forward_hops(r, lambda copy: copy.wait_send())
        return_copy(r).wait_send()
        return carry

    lax.fori_loop(1, nz, drain_column, 0)

    def drain_plane(r, carry):
        over_peers(lambda j: out_copy(r, j).wait_send())
        over_peers(lambda j: back_copy(r, j).wait_send())
        return carry

    lax.fori_loop(0, nz, drain_plane, 0)


def shards(
    residual,
    outer_gate,
    conv_input,
    conv_value,
    doc_ids,
    conv_taps,
    branch_gain,
    out_weight,
    ffn_gain,
    route_ids,
    route_weight,
    shared_gate,
    shared_up,
    shared_down,
    expert_gate,
    expert_up,
    expert_down,
):
    rows, width = residual.shape
    seq_rows, half_width = conv_input.shape
    tops = route_ids.shape[1]
    seq_devices, cores = lax.axis_size("sp"), lax.axis_size("tp")
    nz = column_length(seq_devices)
    plane = seq_devices // nz
    peers = plane * cores
    expert_count = seq_devices * cores
    capacity = rows * cores * tops // expert_count
    slots = -(-capacity // 16) * 16
    lanes = 128
    docs = jnp.broadcast_to(doc_ids.astype(F32)[:, None], (seq_rows, lanes))
    streamed = (
        conv_input,
        conv_value,
        docs,
        route_ids.T,
        route_weight.T,
        outer_gate,
        out_weight,
        residual,
        shared_gate,
        shared_up,
        shared_down,
        expert_gate,
        expert_up,
        expert_down,
    )
    held = [pltpu.VMEM(a.shape, a.dtype) for a in streamed]
    small = (conv_taps, branch_gain, ffn_gain)
    dma = pltpu.SemaphoreType.DMA
    tile = (nz, peers, slots, width)
    lead, packed = 8, 16
    return pl.pallas_call(
        functools.partial(experts_kernel, nz, plane, cores, slots, tops, expert_count),
        out_shape=jax.ShapeDtypeStruct((rows, width), BF16),
        in_specs=[pl.BlockSpec(memory_space=pl.ANY)] * len(streamed)
        + [pl.BlockSpec(memory_space=pltpu.VMEM)] * len(small),
        out_specs=pl.BlockSpec(memory_space=pltpu.VMEM),
        scratch_shapes=[
            *held[:8],
            pltpu.VMEM((lead + seq_rows, half_width), F32),
            pltpu.VMEM((packed, half_width), BF16),
            pltpu.VMEM((packed, half_width), BF16),
            pltpu.VMEM((lead, lanes), F32),
            pltpu.VMEM((seq_rows, half_width), BF16),
            pltpu.VMEM((seq_rows, lanes), F32),
            pltpu.VMEM((rows, half_width), BF16),
            pltpu.VMEM((rows, lanes), F32),
            pltpu.VMEM((nz, rows, width), BF16),
            pltpu.VMEM((nz, 2 * tops, rows), F32),
            pltpu.VMEM(tile, BF16),
            pltpu.VMEM(tile, BF16),
            pltpu.VMEM(tile, BF16),
            pltpu.VMEM(tile, BF16),
            pltpu.VMEM((nz, rows, width), BF16),
            pltpu.VMEM((nz, rows, width), BF16),
            pltpu.VMEM((rows, width), F32),
            *held[8:],
            dma((len(streamed),)),
            dma((3,)),
            dma((3,)),
            dma((2,)),
            dma((2,)),
            dma((2,)),
            dma((2,)),
            dma((nz,)),
            dma((nz,)),
            dma((nz,)),
            dma((nz,)),
            dma((nz, peers)),
            dma((nz, peers)),
            dma((nz, peers)),
            dma((nz, peers)),
            dma((nz,)),
            dma((nz,)),
        ],
        compiler_params=pltpu.CompilerParams(
            collective_id=0, has_side_effects=True, vmem_limit_bytes=67043328
        ),
    )(*streamed, *small)


def solution(mesh):
    placed = (
        P(("sp", "tp"), None),
        P("sp", "tp"),
        P("sp", "tp"),
        P("sp", "tp"),
        P("sp"),
        P(None, "tp"),
        P("tp"),
        P(),
        P(),
        P(("sp", "tp"), None),
        P(("sp", "tp"), None),
        P(),
        P(),
        P(),
        P(("sp", "tp"), None, None),
        P(("sp", "tp"), None, None),
        P(("sp", "tp"), None, None),
    )
    return jax.shard_map(
        shards, mesh=mesh, in_specs=placed, out_specs=P(("sp", "tp"), None), check_vma=False
    )
```
